32 devices in a mesh: kv: 16 (over z, y, core), tp: 2 (over x).
Axes of the slice: x: 2, y: 2, z: 4, core: 2. Of those that a mesh axis runs over, the one named last changes fastest.
Arguments:
- tokens: bfloat16 [6144, 1024], P('kv', 'tp'), may hold values from -6 to 6
- query_weight: bfloat16 [1024, 512], P(None, 'tp'), may hold values from -0.1875 to 0.1875
- key_weight: bfloat16 [1024, 512], P(None, 'tp'), may hold values from -0.1875 to 0.1875
- value_weight: bfloat16 [1024, 512], P(None, 'tp'), may hold values from -0.1875 to 0.1875
- out_weight: bfloat16 [512, 1024], P('tp'), may hold values from -0.25 to 0.25
- norm_gain: float32 [512], P('tp'), may hold values from 0.1 to 1.9
- chosen_owner: int32 [96, 8], P('kv'), may hold values from 0 to 15, all different within a row; in each aligned block of 6 rows (0 to 5, 6 to 11, ...) at most 6 rows name the same one
- chosen_local: int32 [96, 8], P('kv'), may hold values from 0 to 5
Outputs:
- attended_out: bfloat16 [6144, 1024], P('kv', 'tp')
The draws below stay inside these ranges and needn't reach their ends.
Inputs may be any that keep to these rules, and one draw needn't show every extreme that they name: `chosen_owner`: each row names 8 different owners; among the 6 rows of one device no owner is named by more than 6 rows, and in some device's rows one owner is named by exactly 6. `chosen_local`: any index of a key block within its owner.
All inputs are finite; a program needn't handle non-finite values.
Results may differ from the reference program's by a relative error of at most 0.015.
Values may be sent and summed in bfloat16 or wider, within the bound.
A program may use at most 64 MiB of HBM per device.

```python
import math
import jax
import jax.numpy as jnp
import numpy as np
from jax import lax

WIDTH = 1024
HEADS = 8
HEAD_SIZE = 64
BLOCK = 64
CHOSEN = 8
QB_DEV = 6
TOKENS = 6144
BLOCKS_ALL = 96
CAP = 6
N_KV = 16


def with_ends(drawn, key, least, high):
    shape = drawn.shape
    spot = [jax.random.randint(jax.random.fold_in(key, axis), (), 0, shape[axis]) for axis in range(len(shape))]
    drawn = drawn.at[tuple(spot)].set(least)
    longest = shape.index(max(shape))
    spot[longest] = (spot[longest] + 1) % shape[longest]
    return drawn.at[tuple(spot)].set(high)


def level_of(own_key, dims, split, least, largest):
    loudness = 1.0
    for axis_at, shards_of in split:
        draws = jax.random.uniform(jax.random.fold_in(jax.random.fold_in(own_key, 6), axis_at), (shards_of,), jnp.float32, least / len(split), largest / len(split))
        loudness = loudness * jnp.repeat(jnp.exp(draws), dims[axis_at] // shards_of).reshape((-1,) + (1,) * (len(dims) - 1 - axis_at))
    return loudness


def deal_out(key, own, number, rows, amount, top, most, lean):
    sequence = jax.random.permutation(key, amount)
    heavy_load, usual = shares(amount, rows * top, most, lean, True), shares(amount, rows * top, most, lean, False)
    places = jnp.arange(amount)

    def named(sizes, turn):
        used = int((sizes > 0).sum())
        fixed = max(1, used // 4)
        shifted = fixed + (places - fixed + turn * (used - fixed)) % max(1, amount - fixed)
        return jnp.zeros((amount,), jnp.int32).at[sequence[jnp.where(places < fixed, places, shifted)]].set(jnp.asarray(sizes, jnp.int32))

    sizes = jnp.where(number % 4 == 0, named(heavy_load, number // 4), named(usual, number - number // 4 - 1))
    mixed = jax.random.permutation(jax.random.fold_in(own, 3), amount)
    giver, receiver = mixed[0:amount // 2 * 2:2], mixed[1:amount // 2 * 2:2]
    margin = jnp.minimum(sizes[giver] - 1, most - sizes[receiver]) // 2
    margin = jnp.where((giver == sequence[0]) | (receiver == sequence[0]) | (sizes[receiver] == 0), 0, jnp.maximum(margin, 0))
    shifted = jax.random.randint(jax.random.fold_in(own, 4), (amount // 2,), 0, 1 << 20) % (margin + 1)
    sizes = sizes.at[giver].add(-shifted).at[receiver].add(shifted)
    items = jnp.searchsorted(jnp.cumsum(sizes), jnp.arange(rows * top), side="right").astype(jnp.int32)
    listing = items.reshape(top, rows).T
    listing = listing[jax.random.permutation(jax.random.fold_in(own, 1), rows)]
    turn = jax.random.randint(jax.random.fold_in(own, 2), (rows, 1), 0, top)
    return jnp.take_along_axis(listing, (jnp.arange(top)[None, :] + turn) % top, axis=1)


def shares(amount, total, reach, lean, full):
    weights = [(1 << 20) // math.isqrt(grade ** lean) + 1 for grade in range(1, amount + 1)]
    largest = reach if full else min(reach, max(-(-total // amount), total * weights[0] // sum(weights)))
    least = 1 if total - largest >= amount - 1 else 0
    counts, rest = [largest] + [least] * (amount - 1), total - largest - least * (amount - 1)
    while rest > 0:
        candidates = [i for i in range(1, amount) if counts[i] < largest] or [i for i in range(1, amount) if counts[i] < reach]
        mass, left = sum([weights[i] for i in candidates]), rest
        for i in candidates:
            more = min(reach - counts[i], max(1, left * weights[i] // mass), rest)
            counts[i] = counts[i] + more
            rest = rest - more
    return np.array(counts)


def noise(key, shape, scale, limit, shards=(), kind=jnp.bfloat16):
    array = scale * jax.random.normal(key, shape, jnp.float32)
    if shards:
        array = array * level_of(key, shape, shards, -0.22, 0.18)
    return jnp.clip(array, -limit, limit).astype(kind)


def setup_inputs(seed: int = 0) -> dict:
    keys = jax.random.split(jax.random.key(seed), 9)
    tokens = noise(keys[0], (TOKENS, WIDTH), 1.0, 6.0, ((0, 16), (1, 2)))
    query_weight = noise(keys[1], (WIDTH, HEADS * HEAD_SIZE), WIDTH ** -0.5, 0.1875, ((1, 2),))
    key_weight = noise(keys[2], (WIDTH, HEADS * HEAD_SIZE), WIDTH ** -0.5, 0.1875, ((1, 2),))
    value_weight = noise(keys[3], (WIDTH, HEADS * HEAD_SIZE), WIDTH ** -0.5, 0.1875, ((1, 2),))
    out_weight = noise(keys[4], (HEADS * HEAD_SIZE, WIDTH), (HEADS * HEAD_SIZE) ** -0.5, 0.25, ((0, 2),))
    norm_gain = jnp.clip(1.0 + 0.18 * jax.random.normal(keys[5], (HEADS * HEAD_SIZE,), jnp.float32), 0.1, 1.9)
    chosen_owner_keys = jax.random.split(jax.random.fold_in(keys[6], 1), BLOCKS_ALL // QB_DEV)
    chosen_owner_turns = jax.random.permutation(jax.random.fold_in(keys[6], 3), BLOCKS_ALL // QB_DEV)
    chosen_owner = jax.vmap(lambda own, number: deal_out(jax.random.fold_in(keys[6], 2), own, number, QB_DEV, N_KV, CHOSEN, CAP, 2))(chosen_owner_keys, chosen_owner_turns).reshape((BLOCKS_ALL, CHOSEN))
    chosen_local = with_ends(jax.random.randint(keys[7], (BLOCKS_ALL, CHOSEN), 0, QB_DEV), jax.random.fold_in(keys[7], 1), 0, QB_DEV - 1).astype(jnp.int32)
    return dict(tokens=tokens, query_weight=query_weight, key_weight=key_weight, value_weight=value_weight, out_weight=out_weight, norm_gain=norm_gain, chosen_owner=chosen_owner, chosen_local=chosen_local)


neg_fill = -1e+30
eps_norm = 1e-06

def project(tokens, weight):
    return jnp.dot(tokens, weight, preferred_element_type=jnp.float32).astype(jnp.bfloat16)

def reference(tokens, query_weight, key_weight, value_weight, out_weight, norm_gain, chosen_owner, chosen_local):
    block_count = QB_DEV * N_KV
    queries = project(tokens, query_weight).reshape(block_count, BLOCK, HEADS, HEAD_SIZE)
    keys_all = project(tokens, key_weight).reshape(block_count, BLOCK, HEADS, HEAD_SIZE)
    values_all = project(tokens, value_weight).reshape(block_count, BLOCK, HEADS, HEAD_SIZE)
    picked = (chosen_owner * QB_DEV + chosen_local).astype(jnp.int32)
    listed_all = jnp.concatenate([jnp.arange(block_count, dtype=jnp.int32)[:, None], picked], axis=1)
    offsets = jnp.arange(BLOCK, dtype=jnp.int32)
    score_scale = HEAD_SIZE ** (-0.5)
    entry_first = (jnp.arange(CHOSEN + 1, dtype=jnp.int32) == 0)[:, None]

    def attend(packed):
        block_index, listed = packed
        query_rows = queries[block_index].astype(jnp.float32)
        key_rows = keys_all[listed].astype(jnp.float32)
        value_rows = values_all[listed].astype(jnp.float32)
        scores = jnp.einsum('qhd,cthd->hqct', query_rows, key_rows, precision=lax.Precision.HIGHEST) * score_scale
        query_pos = block_index * BLOCK + offsets
        key_pos = jnp.where(entry_first, listed[:, None] * BLOCK + offsets[None, :], jnp.int32(-1))
        visible = key_pos[None, :, :] <= query_pos[:, None, None]
        scores = jnp.where(visible[None], scores, neg_fill)
        highest = lax.optimization_barrier(jnp.max(scores, axis=(2, 3), keepdims=True))
        weights = jnp.where(visible[None], jnp.exp(scores - highest), jnp.float32(0.0))
        mass_sum = lax.optimization_barrier(jnp.sum(weights, axis=(2, 3)))
        blended = jnp.einsum('hqct,cthd->qhd', weights, value_rows, precision=lax.Precision.HIGHEST)
        return (blended / mass_sum.T[:, :, None]).astype(jnp.bfloat16)
    attended = lax.map(attend, (jnp.arange(block_count, dtype=jnp.int32), listed_all))
    attended = attended.reshape(block_count * BLOCK, HEADS * HEAD_SIZE)
    wide_rows = attended.astype(jnp.float32)
    mean_sq = lax.optimization_barrier(jnp.mean(wide_rows * wide_rows, axis=1, keepdims=True))
    normed = (wide_rows * lax.rsqrt(mean_sq + eps_norm) * norm_gain.astype(jnp.float32)).astype(jnp.bfloat16)
    return jnp.dot(normed, out_weight, preferred_element_type=jnp.float32).astype(jnp.bfloat16)
```

```python
import functools

import jax
import jax.numpy as jnp
from jax import lax
from jax.experimental import pallas as pl
from jax.experimental.pallas import tpu as pltpu
from jax.sharding import PartitionSpec as P

HEADS = 8
HEAD_SIZE = 64
BLOCK = 64


neg_fill = -1e30
eps_norm = 1e-06


def folded(value, axis, dim, take_in, carry):
    whole = jax.tree.map(lambda part: lax.all_gather(part, axis, axis=dim, tiled=True), value)
    return take_in(carry, whole, jnp.int32(0))


def for_sending(value):
    return jax.tree.map(lambda a: a.astype(jnp.bfloat16) if a.dtype == jnp.float32 else a, value)


def scattered(portion, width, axis):
    count = width * lax.axis_size(axis)
    sent = portion(jnp.int32(0), count).astype(jnp.bfloat16)
    return lax.psum_scatter(sent, axis, scatter_dimension=0, tiled=True).astype(jnp.float32)


def partial_softmax(query_rows, key_rows, value_rows, query_pos, key_pos):
    score_scale = query_rows.shape[-1] ** (-0.5)
    scores = (
        jnp.einsum("bqhd,bcthd->bhqct", query_rows, key_rows, preferred_element_type=jnp.float32)
        * score_scale
    )
    visible = key_pos[:, None, None, :, :] <= query_pos[:, None, :, None, None]
    scores = jnp.where(visible, scores, neg_fill)
    highest = jnp.max(scores, axis=(3, 4))
    weights = jnp.where(visible, jnp.exp(scores - highest[:, :, :, None, None]), jnp.float32(0.0))
    mass_sum = jnp.sum(weights, axis=(3, 4))
    blended = jnp.einsum(
        "bhqct,bcthd->bqhd",
        weights,
        value_rows.astype(jnp.float32),
        precision=lax.Precision.HIGHEST,
    )
    return (highest, mass_sum, blended)


def on_device(
    tokens,
    query_weight,
    key_weight,
    value_weight,
    out_weight,
    norm_gain,
    chosen_owner,
    chosen_local,
):
    tok_rows = tokens.shape[0]
    blocks_here = tok_rows // BLOCK
    heads_here = query_weight.shape[1] // HEAD_SIZE
    empty_sum = jnp.zeros((tok_rows, query_weight.shape[1]), jnp.float32)

    def add_columns(carried, portion, offset):
        span_rows = portion.shape[1]
        return tuple(
            (
                partial_sum
                + jnp.dot(
                    portion,
                    lax.dynamic_slice_in_dim(weight, offset, span_rows, 0),
                    preferred_element_type=jnp.float32,
                )
                for partial_sum, weight in zip(carried, (query_weight, key_weight, value_weight))
            )
        )

    projected = folded(tokens, "tp", 1, add_columns, (empty_sum, empty_sum, empty_sum))
    local_queries, local_keys, local_values = [
        summed.astype(jnp.bfloat16).reshape(blocks_here, BLOCK, heads_here, HEAD_SIZE)
        for summed in projected
    ]
    device = lax.axis_index("kv")
    kv_count = lax.axis_size("kv")
    chosen_count = chosen_owner.shape[1]
    capacity = min(blocks_here, max(1, 2 * blocks_here * chosen_count // kv_count))
    offsets = jnp.arange(BLOCK, dtype=jnp.int32)
    own_global = device * blocks_here + jnp.arange(blocks_here, dtype=jnp.int32)
    query_pos = own_global[:, None] * BLOCK + offsets[None, :]
    flat_owner = chosen_owner.reshape(-1)
    one_hot = (flat_owner[:, None] == jnp.arange(kv_count, dtype=jnp.int32)[None, :]).astype(
        jnp.int32
    )
    earlier = jnp.cumsum(one_hot, axis=0) - one_hot
    flat_slot = jnp.sum(earlier * one_hot, axis=1)
    requests = (
        jnp.zeros((kv_count, capacity), jnp.int32)
        .at[flat_owner, flat_slot]
        .set(chosen_local.reshape(-1))
    )
    incoming = lax.all_to_all(requests, "kv", split_axis=0, concat_axis=0, tiled=True)
    key_pack = local_keys[incoming]
    value_pack = local_values[incoming]
    key_back, value_back = (
        lax.all_to_all(for_sending(key_pack), "kv", split_axis=0, concat_axis=0, tiled=True).astype(
            key_pack.dtype
        ),
        lax.all_to_all(
            for_sending(value_pack), "kv", split_axis=0, concat_axis=0, tiled=True
        ).astype(value_pack.dtype),
    )
    chosen_keys = key_back[flat_owner, flat_slot].reshape(
        blocks_here, chosen_count, BLOCK, heads_here, HEAD_SIZE
    )
    chosen_values = value_back[flat_owner, flat_slot].reshape(
        blocks_here, chosen_count, BLOCK, heads_here, HEAD_SIZE
    )
    all_keys = jnp.concatenate([local_keys[:, None], chosen_keys], axis=1)
    all_values = jnp.concatenate([local_values[:, None], chosen_values], axis=1)
    own_kpos = (own_global[:, None] * BLOCK + offsets[None, :])[:, None, :]
    chosen_kpos = jnp.full((blocks_here, chosen_count, BLOCK), -1, jnp.int32)
    key_pos = jnp.concatenate([own_kpos, chosen_kpos], axis=1)
    highest, mass_sum, blended = partial_softmax(
        local_queries, all_keys, all_values, query_pos, key_pos
    )
    attended = blended / jnp.transpose(mass_sum, (0, 2, 1))[..., None]
    attended = attended.astype(jnp.bfloat16).reshape(tok_rows, heads_here * HEAD_SIZE)
    wide_rows = attended.astype(jnp.float32)
    squares = lax.psum(jnp.sum(wide_rows * wide_rows, axis=1), "tp")
    mean_sq = squares / (HEADS * HEAD_SIZE)
    normed = (wide_rows * lax.rsqrt(mean_sq + eps_norm)[:, None] * norm_gain).astype(jnp.bfloat16)
    out_cols = out_weight.shape[1] // lax.axis_size("tp")

    def out_term(offset, count):
        columns = lax.dynamic_slice_in_dim(out_weight, offset, count, 1)
        return jnp.einsum("fc,tf->ct", columns, normed, preferred_element_type=jnp.float32)

    summed = scattered(out_term, out_cols, "tp")
    return summed.T.astype(jnp.bfloat16)


MESH_ID = pl.DeviceIdType.MESH
CORES = 2


def kv_grid(kv_count):
    chips = kv_count // CORES
    along_y = 1 << ((chips.bit_length() - 1) // 2)
    return chips // along_y, along_y


def swap_half(value):
    return pltpu.roll(value, value.shape[-1] // 2, 1)


def interleave(first, second):
    low = lax.broadcasted_iota(jnp.int32, first.shape, 1) < first.shape[-1] // 2
    return jnp.where(low, first, swap_half(second)), jnp.where(low, swap_half(first), second)


def fused_kernel(
    nz, ny, tok, wq, wk, wv, wo, gain, owner, local, out,
    tokp, acc, kv, kvs, qs, qbuf, att, ats, wp, gp, cst, cb, cs,
    tok_s, tok_r, w_s, w_r, g_s, g_r, c_s, c_r, zk_s, zk_r, zq_s, zq_r,
    yk_s, yk_r, dk_s, dk_r, rt_s, rt_r, xa_s, xa_r, loc_sem,
):
    me = lax.axis_index("kv")
    x = lax.axis_index("tp")
    z = me // (ny * CORES)
    y = (me // CORES) % ny
    c = me % CORES
    rows, feats = tok.shape
    blocks = rows // BLOCK
    pairs = blocks // 2
    heads = wq.shape[1] // HEAD_SIZE
    hw = heads * HEAD_SIZE
    wide = 2 * HEAD_SIZE
    cols = out.shape[1]

    def dev(zz, yy, cc):
        return (zz * ny + yy) * CORES + cc

    def zfrom(d):
        return (z + nz - d) % nz

    def zto(d):
        return (z + d) % nz

    def push(src, dst, ss, rs, kv_id, tp_id):
        return pltpu.make_async_remote_copy(
            src_ref=src, dst_ref=dst, send_sem=ss, recv_sem=rs,
            device_id={"kv": kv_id, "tp": tp_id}, device_id_type=MESH_ID,
        )

    barrier = pltpu.get_barrier_semaphore()
    peers = [(me, 1 - x), (dev(z, 1 - y, c), x), (dev(z, y, 1 - c), x)]
    peers += [(dev(zto(d), y, c), x) for d in range(1, nz)]
    for kv_id, tp_id in peers:
        pl.semaphore_signal(
            barrier, inc=1, device_id={"kv": kv_id, "tp": tp_id}, device_id_type=MESH_ID
        )
    cst[...] = jnp.zeros(cst.shape, jnp.int32)
    cst[0:blocks, 0 : owner.shape[1]] = owner[...] * blocks + local[...]
    pl.semaphore_wait(barrier, len(peers))

    def tok_copy(k):
        part = pl.ds(k * 2 * BLOCK, 2 * BLOCK)
        return push(tok.at[part], tokp.at[part], tok_s.at[k], tok_r.at[k], me, 1 - x)

    def w_copy():
        theirs = pl.ds(pl.multiple_of((1 - x) * cols, 128), cols)
        return push(wo.at[:, theirs], wp, w_s, w_r, me, 1 - x)

    def g_copy():
        return push(gain, gp, g_s, g_r, me, 1 - x)

    def c_copy(d):
        return push(cst, cb.at[d], c_s.at[d], c_r.at[d], dev(zto(d), y, c), x)

    def zk_copy(d, k):
        part = pl.ds(2 * k, 2)
        return push(
            kvs.at[zto(d), part], kv.at[pl.ds(me * blocks + 2 * k, 2)],
            zk_s.at[d, k], zk_r.at[d, k], dev(zto(d), y, c), x,
        )

    def zq_copy(d, k):
        return push(
            qs.at[zto(d), k], qbuf.at[d, k], zq_s.at[d, k], zq_r.at[d, k], dev(zto(d), y, c), x
        )

    def slot(d, yy, k):
        return kv.at[pl.ds(dev(zfrom(d), yy, c) * blocks + 2 * k, 2)]

    def yk_copy(d, k):
        part = slot(d, y, k)
        return push(part, part, yk_s.at[d, k], yk_r.at[d, k], dev(z, 1 - y, c), x)

    def dk_copy(side, d, k):
        part = slot(d, y if side == 0 else 1 - y, k)
        return push(
            part, part, dk_s.at[side, d, k], dk_r.at[side, d, k], dev(z, y, 1 - c), x
        )

    def rt_copy(d, p):
        return push(
            ats.at[d, p], att.at[x, z, p], rt_s.at[d, p], rt_r.at[d, p], dev(zfrom(d), y, c), x
        )

    def xa_copy(d, p):
        part = att.at[x, zto(d), p]
        return push(part, part, xa_s.at[d, p], xa_r.at[d, p], me, 1 - x)

    for k in range(pairs):
        tok_copy(k).start()
    w_copy().start()
    g_copy().start()
    for d in range(1, nz):
        c_copy(d).start()
    cb[0] = cst[...]

    mine = pl.ds(pl.multiple_of(x * feats, 128), feats)
    theirs = pl.ds(pl.multiple_of((1 - x) * feats, 128), feats)
    for at, weight in enumerate((wq, wk, wv)):
        acc[:, at * hw : (at + 1) * hw] = jnp.dot(
            tok[...], weight[mine, :], preferred_element_type=jnp.float32
        )

    scale = HEAD_SIZE**-0.5
    for k in range(pairs):
        tok_copy(k).wait_recv()
        span = slice(2 * k * BLOCK, (2 * k + 2) * BLOCK)
        got = []
        for at, weight in enumerate((wq, wk, wv)):
            got.append(
                acc[span, at * hw : (at + 1) * hw]
                + jnp.dot(
                    tokp[span, :], weight[theirs, :], preferred_element_type=jnp.float32
                )
            )
        q, key, val = got
        for j in range(heads // 2):
            lanes = slice(j * wide, (j + 1) * wide)
            even, odd = interleave(key[:, lanes], val[:, lanes])
            for h, both in ((2 * j, even), (2 * j + 1, odd)):
                kvs[h, 2 * k : 2 * k + 2] = both.astype(jnp.bfloat16).reshape(2, BLOCK, wide)
        kv[pl.ds(me * blocks + 2 * k, 2)] = kvs[z, 2 * k : 2 * k + 2]
        for d in sorted(range(1, nz), key=lambda d: abs(2 * d - nz)):
            zk_copy(d, k).start()
        yk_copy(0, k).start()
        dk_copy(0, 0, k).start()
        for j in range(heads // 2):
            lanes = slice(j * wide, (j + 1) * wide)
            even, odd = interleave(q[:BLOCK, lanes], q[BLOCK:, lanes])
            qs[2 * j, k] = (even.astype(jnp.bfloat16) * scale).astype(jnp.bfloat16)
            qs[2 * j + 1, k] = (odd.astype(jnp.bfloat16) * scale).astype(jnp.bfloat16)
        qbuf[0, k] = qs[z, k]
        for d in range(1, nz):
            zq_copy(d, k).start()

    order = [(d, k) for k in range(pairs) for d in range(nz)]
    lag = nz
    for at in range(len(order) + lag):
        if at < len(order):
            d, k = order[at]
            if d > 0:
                zk_copy(d, k).wait_recv()
                yk_copy(d, k).start()
                dk_copy(0, d, k).start()
        if at >= lag:
            d, k = order[at - lag]
            yk_copy(d, k).wait_recv()
            dk_copy(1, d, k).start()
    for d in range(1, nz):
        c_copy(d).wait_recv()
        for k in range(pairs):
            zq_copy(d, k).wait_recv()
    to_scalar = pltpu.make_async_copy(cb, cs, loc_sem)
    to_scalar.start()
    to_scalar.wait()
    for d, k in order:
        for side in range(2):
            dk_copy(side, d, k).wait_recv()

    chosen = owner.shape[1]
    listed = (chosen + 1) * BLOCK
    row_at = lax.broadcasted_iota(jnp.int32, (BLOCK, listed), 0)
    col_at = lax.broadcasted_iota(jnp.int32, (BLOCK, listed), 1)
    visible = (col_at <= row_at) | (col_at >= BLOCK)
    low = lax.broadcasted_iota(jnp.int32, (BLOCK, wide), 1) < HEAD_SIZE

    def attend(query, d, b):
        own = dev(zfrom(d), y, c) * blocks + b
        pieces = [kv[own]] + [kv[cs[d, b, j]] for j in range(chosen)]
        both = jnp.concatenate(pieces, axis=0)
        scores = lax.dot_general(
            query, both, (((1,), (1,)), ((), ())), preferred_element_type=jnp.float32
        )
        scores = jnp.where(visible, scores, neg_fill)
        highest = jnp.max(scores, axis=1, keepdims=True)
        weights = jnp.exp(scores - highest)
        mass = jnp.sum(weights, axis=1, keepdims=True)
        blended = jnp.dot(weights.astype(jnp.bfloat16), both, preferred_element_type=jnp.float32)
        return blended / mass

    def pair_of(d, p):
        packed = qbuf[d, p].astype(jnp.float32)
        nothing = jnp.zeros_like(packed)
        first = jnp.where(low, packed, nothing).astype(jnp.bfloat16)
        second = jnp.where(low, swap_half(packed), nothing).astype(jnp.bfloat16)
        first = attend(first, d, 2 * p)
        second = attend(second, d, 2 * p + 1)
        return jnp.where(low, swap_half(first), second).astype(jnp.bfloat16)

    def pass_on(d):
        for p in range(pairs):
            rt_copy(d, p).wait_recv()
            xa_copy(d, p).start()

    sequence = list(range(nz - 1, -1, -1))
    for turn, d in enumerate(sequence):

        def one(p, carry, d=d):
            if d == 0:
                att[x, z, p] = pair_of(d, p)
                xa_copy(d, p).start()
            else:
                ats[d, p] = pair_of(d, p)
                rt_copy(d, p).start()
            return carry

        lax.fori_loop(0, pairs, one, 0)
        if turn >= 2:
            pass_on(sequence[turn - 2])
    for d in sequence[-2:]:
        if d > 0:
            pass_on(d)

    w_copy().wait_recv()
    g_copy().wait_recv()
    mine_cols = pl.ds(pl.multiple_of(x * cols, 128), cols)
    for p in range(pairs):
        for d in range(nz):
            xa_copy(d, p).wait_recv()
        halves = []
        for side in (x, 1 - x):
            upper, lower = [], []
            for j in range(heads // 2):
                up, down = interleave(
                    att[side, 2 * j, p].astype(jnp.float32),
                    att[side, 2 * j + 1, p].astype(jnp.float32),
                )
                upper.append(up)
                lower.append(down)
            halves.append(
                jnp.concatenate(
                    [jnp.concatenate(upper, axis=1), jnp.concatenate(lower, axis=1)], axis=0
                )
            )
        squares = sum(jnp.sum(half * half, axis=1, keepdims=True) for half in halves)
        inverse = lax.rsqrt(squares / (2 * hw) + eps_norm)
        normed = [
            (half * inverse * g[...]).astype(jnp.bfloat16) for half, g in zip(halves, (gain, gp))
        ]
        total = jnp.dot(normed[0], wo[:, mine_cols], preferred_element_type=jnp.float32)
        total += jnp.dot(normed[1], wp[...], preferred_element_type=jnp.float32)
        out[2 * p * BLOCK : (2 * p + 2) * BLOCK, :] = total.astype(jnp.bfloat16)

    for k in range(pairs):
        tok_copy(k).wait_send()
    w_copy().wait_send()
    g_copy().wait_send()
    for d in range(nz):
        if d > 0:
            c_copy(d).wait_send()
        for k in range(pairs):
            if d > 0:
                zk_copy(d, k).wait_send()
                zq_copy(d, k).wait_send()
                rt_copy(d, k).wait_send()
            yk_copy(d, k).wait_send()
            dk_copy(0, d, k).wait_send()
            dk_copy(1, d, k).wait_send()
            xa_copy(d, k).wait_send()


def fused(nz, ny, tok, wq, wk, wv, wo, gain, owner, local):
    rows, feats = tok.shape
    blocks = rows // BLOCK
    pairs = blocks // 2
    heads = wq.shape[1] // HEAD_SIZE
    hw = heads * HEAD_SIZE
    cols = wo.shape[1] // 2
    wide = 2 * HEAD_SIZE
    everyone = nz * ny * CORES * blocks
    bf16 = jnp.bfloat16
    vmem, dma = pltpu.VMEM, pltpu.SemaphoreType.DMA
    two = lambda shape: [dma(shape), dma(shape)]
    scratch = [
        vmem((rows, feats), bf16),
        vmem((rows, 3 * hw), jnp.float32),
        vmem((everyone, BLOCK, wide), bf16),
        vmem((heads, blocks, BLOCK, wide), bf16),
        vmem((heads, pairs, BLOCK, wide), bf16),
        vmem((nz, pairs, BLOCK, wide), bf16),
        vmem((2, heads, pairs, BLOCK, wide), bf16),
        vmem((nz, pairs, BLOCK, wide), bf16),
        vmem((hw, cols), bf16),
        vmem((1, hw), jnp.float32),
        vmem((8, 128), jnp.int32),
        vmem((nz, 8, 128), jnp.int32),
        pltpu.SMEM((nz, 8, 128), jnp.int32),
    ]
    scratch += two((pairs,)) + two(()) + two(()) + two((nz,))
    scratch += two((nz, pairs)) * 3 + two((2, nz, pairs)) + two((nz, pairs)) * 2 + [dma(())]
    return pl.pallas_call(
        functools.partial(fused_kernel, nz, ny),
        out_shape=jax.ShapeDtypeStruct((rows, cols), bf16),
        in_specs=[pl.BlockSpec(memory_space=pltpu.VMEM)] * 8,
        out_specs=pl.BlockSpec(memory_space=pltpu.VMEM),
        scratch_shapes=scratch,
        compiler_params=pltpu.CompilerParams(collective_id=0, has_side_effects=True),
    )(tok, wq, wk, wv, wo, gain.reshape(1, hw), owner, local)


def solution(mesh):
    kv_count, tp_count = mesh.shape["kv"], mesh.shape["tp"]
    nz, ny = kv_grid(kv_count)

    def step(tokens, *rest):
        blocks = tokens.shape[0] // BLOCK
        heads = rest[0].shape[1] // HEAD_SIZE
        fits = (
            tp_count == 2 and ny == 2 and nz == heads and blocks % 2 == 0 and blocks <= 8
            and nz * ny * CORES == kv_count and 2 * HEAD_SIZE == 128
        )
        if fits:
            return fused(nz, ny, tokens, *rest)
        return on_device(tokens, *rest)

    return jax.shard_map(
        step,
        mesh=mesh,
        in_specs=(
            P("kv", "tp"),
            P(None, "tp"),
            P(None, "tp"),
            P(None, "tp"),
            P("tp", None),
            P("tp"),
            P("kv", None),
            P("kv", None),
        ),
        out_specs=P("kv", "tp"),
        check_vma=False,
    )
```

```python
import functools

import jax
import jax.numpy as jnp
from jax import lax
from jax.experimental import pallas as pl
from jax.experimental.pallas import tpu as pltpu
from jax.sharding import PartitionSpec as P

HEADS = 8
HEAD_SIZE = 64
BLOCK = 64


neg_fill = -1e30
eps_norm = 1e-06


def folded(value, axis, dim, take_in, carry):
    whole = jax.tree.map(lambda part: lax.all_gather(part, axis, axis=dim, tiled=True), value)
    return take_in(carry, whole, jnp.int32(0))


def for_sending(value):
    return jax.tree.map(lambda a: a.astype(jnp.bfloat16) if a.dtype == jnp.float32 else a, value)


def scattered(portion, width, axis):
    count = width * lax.axis_size(axis)
    sent = portion(jnp.int32(0), count).astype(jnp.bfloat16)
    return lax.psum_scatter(sent, axis, scatter_dimension=0, tiled=True).astype(jnp.float32)


def partial_softmax(query_rows, key_rows, value_rows, query_pos, key_pos):
    score_scale = query_rows.shape[-1] ** (-0.5)
    scores = (
        jnp.einsum("bqhd,bcthd->bhqct", query_rows, key_rows, preferred_element_type=jnp.float32)
        * score_scale
    )
    visible = key_pos[:, None, None, :, :] <= query_pos[:, None, :, None, None]
    scores = jnp.where(visible, scores, neg_fill)
    highest = jnp.max(scores, axis=(3, 4))
    weights = jnp.where(visible, jnp.exp(scores - highest[:, :, :, None, None]), jnp.float32(0.0))
    mass_sum = jnp.sum(weights, axis=(3, 4))
    blended = jnp.einsum(
        "bhqct,bcthd->bqhd",
        weights,
        value_rows.astype(jnp.float32),
        precision=lax.Precision.HIGHEST,
    )
    return (highest, mass_sum, blended)


def on_device(
    tokens,
    query_weight,
    key_weight,
    value_weight,
    out_weight,
    norm_gain,
    chosen_owner,
    chosen_local,
):
    tok_rows = tokens.shape[0]
    blocks_here = tok_rows // BLOCK
    heads_here = query_weight.shape[1] // HEAD_SIZE
    empty_sum = jnp.zeros((tok_rows, query_weight.shape[1]), jnp.float32)

    def add_columns(carried, portion, offset):
        span_rows = portion.shape[1]
        return tuple(
            (
                partial_sum
                + jnp.dot(
                    portion,
                    lax.dynamic_slice_in_dim(weight, offset, span_rows, 0),
                    preferred_element_type=jnp.float32,
                )
                for partial_sum, weight in zip(carried, (query_weight, key_weight, value_weight))
            )
        )

    projected = folded(tokens, "tp", 1, add_columns, (empty_sum, empty_sum, empty_sum))
    local_queries, local_keys, local_values = [
        summed.astype(jnp.bfloat16).reshape(blocks_here, BLOCK, heads_here, HEAD_SIZE)
        for summed in projected
    ]
    device = lax.axis_index("kv")
    kv_count = lax.axis_size("kv")
    chosen_count = chosen_owner.shape[1]
    capacity = min(blocks_here, max(1, 2 * blocks_here * chosen_count // kv_count))
    offsets = jnp.arange(BLOCK, dtype=jnp.int32)
    own_global = device * blocks_here + jnp.arange(blocks_here, dtype=jnp.int32)
    query_pos = own_global[:, None] * BLOCK + offsets[None, :]
    flat_owner = chosen_owner.reshape(-1)
    one_hot = (flat_owner[:, None] == jnp.arange(kv_count, dtype=jnp.int32)[None, :]).astype(
        jnp.int32
    )
    earlier = jnp.cumsum(one_hot, axis=0) - one_hot
    flat_slot = jnp.sum(earlier * one_hot, axis=1)
    requests = (
        jnp.zeros((kv_count, capacity), jnp.int32)
        .at[flat_owner, flat_slot]
        .set(chosen_local.reshape(-1))
    )
    incoming = lax.all_to_all(requests, "kv", split_axis=0, concat_axis=0, tiled=True)
    key_pack = local_keys[incoming]
    value_pack = local_values[incoming]
    key_back, value_back = (
        lax.all_to_all(for_sending(key_pack), "kv", split_axis=0, concat_axis=0, tiled=True).astype(
            key_pack.dtype
        ),
        lax.all_to_all(
            for_sending(value_pack), "kv", split_axis=0, concat_axis=0, tiled=True
        ).astype(value_pack.dtype),
    )
    chosen_keys = key_back[flat_owner, flat_slot].reshape(
        blocks_here, chosen_count, BLOCK, heads_here, HEAD_SIZE
    )
    chosen_values = value_back[flat_owner, flat_slot].reshape(
        blocks_here, chosen_count, BLOCK, heads_here, HEAD_SIZE
    )
    all_keys = jnp.concatenate([local_keys[:, None], chosen_keys], axis=1)
    all_values = jnp.concatenate([local_values[:, None], chosen_values], axis=1)
    own_kpos = (own_global[:, None] * BLOCK + offsets[None, :])[:, None, :]
    chosen_kpos = jnp.full((blocks_here, chosen_count, BLOCK), -1, jnp.int32)
    key_pos = jnp.concatenate([own_kpos, chosen_kpos], axis=1)
    highest, mass_sum, blended = partial_softmax(
        local_queries, all_keys, all_values, query_pos, key_pos
    )
    attended = blended / jnp.transpose(mass_sum, (0, 2, 1))[..., None]
    attended = attended.astype(jnp.bfloat16).reshape(tok_rows, heads_here * HEAD_SIZE)
    wide_rows = attended.astype(jnp.float32)
    squares = lax.psum(jnp.sum(wide_rows * wide_rows, axis=1), "tp")
    mean_sq = squares / (HEADS * HEAD_SIZE)
    normed = (wide_rows * lax.rsqrt(mean_sq + eps_norm)[:, None] * norm_gain).astype(jnp.bfloat16)
    out_cols = out_weight.shape[1] // lax.axis_size("tp")

    def out_term(offset, count):
        columns = lax.dynamic_slice_in_dim(out_weight, offset, count, 1)
        return jnp.einsum("fc,tf->ct", columns, normed, preferred_element_type=jnp.float32)

    summed = scattered(out_term, out_cols, "tp")
    return summed.T.astype(jnp.bfloat16)


MESH_ID = pl.DeviceIdType.MESH
CORES = 2


def kv_grid(kv_count):
    chips = kv_count // CORES
    along_y = 1 << ((chips.bit_length() - 1) // 2)
    return chips // along_y, along_y


def chunk_spans(blocks):
    return [(0, 1), (1, 1)] + [(b, 2) for b in range(2, blocks, 2)]


def swap_half(value):
    return pltpu.roll(value, value.shape[-1] // 2, 1)


def interleave(first, second):
    low = lax.broadcasted_iota(jnp.int32, first.shape, 1) < first.shape[-1] // 2
    return jnp.where(low, first, swap_half(second)), jnp.where(low, swap_half(first), second)


def fused_kernel(
    nz, ny, tok, wq, wk, wv, wo, gain, owner, local, out,
    tokp, acc, kv, kvs, qs, qbuf, att, ats, wp, gp, cst, cb, cs,
    tok_s, tok_r, w_s, w_r, g_s, g_r, c_s, c_r, zk_s, zk_r, zq_s, zq_r,
    yk_s, yk_r, dk_s, dk_r, rt_s, rt_r, xa_s, xa_r, loc_sem,
):
    me = lax.axis_index("kv")
    x = lax.axis_index("tp")
    z = me // (ny * CORES)
    y = (me // CORES) % ny
    c = me % CORES
    rows, feats = tok.shape
    blocks = rows // BLOCK
    pairs = blocks // 2
    spans = chunk_spans(blocks)
    chunks = range(len(spans))
    heads = wq.shape[1] // HEAD_SIZE
    hw = heads * HEAD_SIZE
    wide = 2 * HEAD_SIZE
    cols = out.shape[1]

    def dev(zz, yy, cc):
        return (zz * ny + yy) * CORES + cc

    def zfrom(d):
        return (z + nz - d) % nz

    def zto(d):
        return (z + d) % nz

    def push(src, dst, ss, rs, kv_id, tp_id):
        return pltpu.make_async_remote_copy(
            src_ref=src, dst_ref=dst, send_sem=ss, recv_sem=rs,
            device_id={"kv": kv_id, "tp": tp_id}, device_id_type=MESH_ID,
        )

    barrier = pltpu.get_barrier_semaphore()
    peers = [(me, 1 - x), (dev(z, 1 - y, c), x), (dev(z, y, 1 - c), x)]
    peers += [(dev(zto(d), y, c), x) for d in range(1, nz)]
    for kv_id, tp_id in peers:
        pl.semaphore_signal(
            barrier, inc=1, device_id={"kv": kv_id, "tp": tp_id}, device_id_type=MESH_ID
        )
    cst[...] = jnp.zeros(cst.shape, jnp.int32)
    cst[0:blocks, 0 : owner.shape[1]] = owner[...] * blocks + local[...]
    mine = pl.ds(pl.multiple_of(x * feats, 128), feats)
    theirs = pl.ds(pl.multiple_of((1 - x) * feats, 128), feats)
    for at, weight in enumerate((wq, wk, wv)):
        acc[:, at * hw : (at + 1) * hw] = jnp.dot(
            tok[...], weight[mine, :], preferred_element_type=jnp.float32
        )
    pl.semaphore_wait(barrier, len(peers))

    def tok_copy(k):
        part = pl.ds(spans[k][0] * BLOCK, spans[k][1] * BLOCK)
        return push(tok.at[part], tokp.at[part], tok_s.at[k], tok_r.at[k], me, 1 - x)

    def w_copy():
        theirs = pl.ds(pl.multiple_of((1 - x) * cols, 128), cols)
        return push(wo.at[:, theirs], wp, w_s, w_r, me, 1 - x)

    def g_copy():
        return push(gain, gp, g_s, g_r, me, 1 - x)

    def c_copy(d):
        return push(cst, cb.at[d], c_s.at[d], c_r.at[d], dev(zto(d), y, c), x)

    def zk_copy(d, k):
        at, many = spans[k]
        return push(
            kvs.at[zto(d), pl.ds(at, many)], kv.at[pl.ds(me * blocks + at, many)],
            zk_s.at[d, k], zk_r.at[d, k], dev(zto(d), y, c), x,
        )

    def zq_copy(d):
        return push(qs.at[zto(d)], qbuf.at[d], zq_s.at[d], zq_r.at[d], dev(zto(d), y, c), x)

    def slot(d, yy, k):
        return kv.at[pl.ds(dev(zfrom(d), yy, c) * blocks + spans[k][0], spans[k][1])]

    def yk_copy(d, k):
        part = slot(d, y, k)
        return push(part, part, yk_s.at[d, k], yk_r.at[d, k], dev(z, 1 - y, c), x)

    def dk_copy(side, d, k):
        part = slot(d, y if side == 0 else 1 - y, k)
        return push(
            part, part, dk_s.at[side, d, k], dk_r.at[side, d, k], dev(z, y, 1 - c), x
        )

    def rt_copy(d, p):
        return push(
            ats.at[d, p], att.at[x, z, p], rt_s.at[d, p], rt_r.at[d, p], dev(zfrom(d), y, c), x
        )

    def xa_copy(d, p):
        part = att.at[x, zto(d), p]
        return push(part, part, xa_s.at[d, p], xa_r.at[d, p], me, 1 - x)

    for k in chunks:
        tok_copy(k).start()
    w_copy().start()
    g_copy().start()
    for d in range(1, nz):
        c_copy(d).start()
    cb[0] = cst[...]

    scale = HEAD_SIZE**-0.5
    far_first = sorted(range(1, nz), key=lambda d: abs(2 * d - nz))

    def rest(at, weight, span):
        return acc[span, at * hw : (at + 1) * hw] + jnp.dot(
            tokp[span, :], weight[theirs, :], preferred_element_type=jnp.float32
        )

    def keys_out(k):
        at, many = spans[k]
        tok_copy(k).wait_recv()
        span = slice(at * BLOCK, (at + many) * BLOCK)
        key, val = rest(1, wk, span), rest(2, wv, span)
        for j in range(heads // 2):
            lanes = slice(j * wide, (j + 1) * wide)
            even, odd = interleave(key[:, lanes], val[:, lanes])
            for h, both in ((2 * j, even), (2 * j + 1, odd)):
                kvs[h, at : at + many] = both.astype(jnp.bfloat16).reshape(many, BLOCK, wide)
        for d in far_first:
            zk_copy(d, k).start()
        kv[pl.ds(me * blocks + at, many)] = kvs[z, at : at + many]
        yk_copy(0, k).start()
        dk_copy(0, 0, k).start()

    def queries_out():
        q = rest(0, wq, slice(0, rows))
        for j in range(heads // 2):
            lanes = slice(j * wide, (j + 1) * wide)
            for k in range(pairs):
                first = q[2 * k * BLOCK : (2 * k + 1) * BLOCK, lanes]
                second = q[(2 * k + 1) * BLOCK : (2 * k + 2) * BLOCK, lanes]
                even, odd = interleave(first, second)
                qs[2 * j, k] = (even.astype(jnp.bfloat16) * scale).astype(jnp.bfloat16)
                qs[2 * j + 1, k] = (odd.astype(jnp.bfloat16) * scale).astype(jnp.bfloat16)
        for d in far_first:
            zq_copy(d).start()
        qbuf[0] = qs[z]

    def relay_z(k):
        for d in range(1, nz):
            zk_copy(d, k).wait_recv()
            yk_copy(d, k).start()
            dk_copy(0, d, k).start()

    def relay_y(k):
        for d in range(nz):
            yk_copy(d, k).wait_recv()
            dk_copy(1, d, k).start()

    last = len(spans) - 1
    for k in chunks:
        keys_out(k)
        if k >= 2:
            relay_z(k - 2)
    queries_out()
    for k in range(max(0, last - 1), last + 1):
        relay_z(k)
        if k >= 1:
            relay_y(k - 1)
        if k == last - 1:
            for early in range(k - 1):
                relay_y(early)
    relay_y(last)
    for d in range(1, nz):
        c_copy(d).wait_recv()
    to_scalar = pltpu.make_async_copy(cb, cs, loc_sem)
    to_scalar.start()
    to_scalar.wait()
    for d in range(1, nz):
        zq_copy(d).wait_recv()
    for k in chunks:
        for d in range(nz):
            for side in range(2):
                dk_copy(side, d, k).wait_recv()

    chosen = owner.shape[1]
    listed = (chosen + 1) * BLOCK
    row_at = lax.broadcasted_iota(jnp.int32, (BLOCK, listed), 0)
    col_at = lax.broadcasted_iota(jnp.int32, (BLOCK, listed), 1)
    visible = (col_at <= row_at) | (col_at >= BLOCK)
    low = lax.broadcasted_iota(jnp.int32, (BLOCK, wide), 1) < HEAD_SIZE

    def attend(query, d, b):
        own = dev(zfrom(d), y, c) * blocks + b
        pieces = [kv[own]] + [kv[cs[d, b, j]] for j in range(chosen)]
        both = jnp.concatenate(pieces, axis=0)
        scores = lax.dot_general(
            query, both, (((1,), (1,)), ((), ())), preferred_element_type=jnp.float32
        )
        scores = jnp.where(visible, scores, neg_fill)
        highest = jnp.max(scores, axis=1, keepdims=True)
        weights = jnp.exp(scores - highest)
        mass = jnp.sum(weights, axis=1, keepdims=True)
        blended = jnp.dot(weights.astype(jnp.bfloat16), both, preferred_element_type=jnp.float32)
        return blended / mass

    def pair_of(d, p):
        packed = qbuf[d, p].astype(jnp.float32)
        nothing = jnp.zeros_like(packed)
        first = jnp.where(low, packed, nothing).astype(jnp.bfloat16)
        second = jnp.where(low, swap_half(packed), nothing).astype(jnp.bfloat16)
        first = attend(first, d, 2 * p)
        second = attend(second, d, 2 * p + 1)
        return jnp.where(low, swap_half(first), second).astype(jnp.bfloat16)

    sequence = list(range(nz - 1, -1, -1))

    def work(p):
        for at in range(0, nz, 2):
            group = sequence[at : at + 2]
            done = [pair_of(d, p) for d in group]
            for d, value in zip(group, done):
                if d == 0:
                    att[x, z, p] = value
                    xa_copy(d, p).start()
                else:
                    ats[d, p] = value
                    rt_copy(d, p).start()

    def pass_on(p):
        for d in sequence[:-1]:
            rt_copy(d, p).wait_recv()
            xa_copy(d, p).start()

    mine_cols = pl.ds(pl.multiple_of(x * cols, 128), cols)

    def finish(p):
        for d in range(nz):
            xa_copy(d, p).wait_recv()
        halves = []
        for side in (x, 1 - x):
            upper, lower = [], []
            for j in range(heads // 2):
                up, down = interleave(
                    att[side, 2 * j, p].astype(jnp.float32),
                    att[side, 2 * j + 1, p].astype(jnp.float32),
                )
                upper.append(up)
                lower.append(down)
            halves.append(
                jnp.concatenate(
                    [jnp.concatenate(upper, axis=1), jnp.concatenate(lower, axis=1)], axis=0
                )
            )
        squares = sum(jnp.sum(half * half, axis=1, keepdims=True) for half in halves)
        inverse = lax.rsqrt(squares / (2 * hw) + eps_norm)
        normed = [
            (half * inverse * g[...]).astype(jnp.bfloat16) for half, g in zip(halves, (gain, gp))
        ]
        total = jnp.dot(normed[0], wo[:, mine_cols], preferred_element_type=jnp.float32)
        total += jnp.dot(normed[1], wp[...], preferred_element_type=jnp.float32)
        out[2 * p * BLOCK : (2 * p + 2) * BLOCK, :] = total.astype(jnp.bfloat16)

    for p in range(pairs):
        work(p)
        if p >= 1:
            pass_on(p - 1)
    w_copy().wait_recv()
    g_copy().wait_recv()
    for p in range(pairs - 1):
        finish(p)
        if p == pairs - 2:
            pass_on(pairs - 1)
    if pairs == 1:
        pass_on(0)
    finish(pairs - 1)

    for k in chunks:
        tok_copy(k).wait_send()
    w_copy().wait_send()
    g_copy().wait_send()
    for d in range(nz):
        if d > 0:
            c_copy(d).wait_send()
            zq_copy(d).wait_send()
        for k in chunks:
            if d > 0:
                zk_copy(d, k).wait_send()
            yk_copy(d, k).wait_send()
            dk_copy(0, d, k).wait_send()
            dk_copy(1, d, k).wait_send()
        for p in range(pairs):
            if d > 0:
                rt_copy(d, p).wait_send()
            xa_copy(d, p).wait_send()


def fused(nz, ny, tok, wq, wk, wv, wo, gain, owner, local):
    rows, feats = tok.shape
    blocks = rows // BLOCK
    pairs = blocks // 2
    heads = wq.shape[1] // HEAD_SIZE
    hw = heads * HEAD_SIZE
    cols = wo.shape[1] // 2
    wide = 2 * HEAD_SIZE
    everyone = nz * ny * CORES * blocks
    bf16 = jnp.bfloat16
    vmem, dma = pltpu.VMEM, pltpu.SemaphoreType.DMA
    two = lambda shape: [dma(shape), dma(shape)]
    scratch = [
        vmem((rows, feats), bf16),
        vmem((rows, 3 * hw), jnp.float32),
        vmem((everyone, BLOCK, wide), bf16),
        vmem((heads, blocks, BLOCK, wide), bf16),
        vmem((heads, pairs, BLOCK, wide), bf16),
        vmem((nz, pairs, BLOCK, wide), bf16),
        vmem((2, heads, pairs, BLOCK, wide), bf16),
        vmem((nz, pairs, BLOCK, wide), bf16),
        vmem((hw, cols), bf16),
        vmem((1, hw), jnp.float32),
        vmem((8, 128), jnp.int32),
        vmem((nz, 8, 128), jnp.int32),
        pltpu.SMEM((nz, 8, 128), jnp.int32),
    ]
    many = len(chunk_spans(blocks))
    scratch += two((many,)) + two(()) + two(()) + two((nz,))
    scratch += two((nz, many)) + two((nz,)) + two((nz, many)) + two((2, nz, many))
    scratch += two((nz, pairs)) * 2 + [dma(())]
    return pl.pallas_call(
        functools.partial(fused_kernel, nz, ny),
        out_shape=jax.ShapeDtypeStruct((rows, cols), bf16),
        in_specs=[pl.BlockSpec(memory_space=pltpu.VMEM)] * 8,
        out_specs=pl.BlockSpec(memory_space=pltpu.VMEM),
        scratch_shapes=scratch,
        compiler_params=pltpu.CompilerParams(collective_id=0, has_side_effects=True),
    )(tok, wq, wk, wv, wo, gain.reshape(1, hw), owner, local)


def solution(mesh):
    kv_count, tp_count = mesh.shape["kv"], mesh.shape["tp"]
    nz, ny = kv_grid(kv_count)

    def step(tokens, *rest):
        blocks = tokens.shape[0] // BLOCK
        heads = rest[0].shape[1] // HEAD_SIZE
        fits = (
            tp_count == 2 and ny == 2 and nz == heads and blocks % 2 == 0 and blocks <= 8
            and nz * ny * CORES == kv_count and 2 * HEAD_SIZE == 128
        )
        if fits:
            return fused(nz, ny, tokens, *rest)
        return on_device(tokens, *rest)

    return jax.shard_map(
        step,
        mesh=mesh,
        in_specs=(
            P("kv", "tp"),
            P(None, "tp"),
            P(None, "tp"),
            P(None, "tp"),
            P("tp", None),
            P("tp"),
            P("kv", None),
            P("kv", None),
        ),
        out_specs=P("kv", "tp"),
        check_vma=False,
    )
```
